32 devices in a mesh: rep: 2 (over y), fs: 4 (over z), tp: 4 (over x, core).
Axes of the slice: x: 2, y: 2, z: 4, core: 2. Of those that a mesh axis runs over, the one named last changes fastest.
Arguments:
- stream: bfloat16 [2048, 2048], P(('rep', 'fs')), may hold values from -6 to 6
- gain_mix: float32 [2048], replicated, may hold values from 0.1 to 1.9
- w_query: float32 [2048, 2048], P('fs', 'tp'), may hold values from -0.125 to 0.125
- scale_query: float32 [2048], P('tp'), may hold values from 0.5 to 2
- w_key: float32 [2048, 2048], P('fs', 'tp'), may hold values from -0.125 to 0.125
- scale_key: float32 [2048], P('tp'), may hold values from 0.5 to 2
- w_value: float32 [2048, 2048], P('fs', 'tp'), may hold values from -0.125 to 0.125
- scale_value: float32 [2048], P('tp'), may hold values from 0.5 to 2
- gain_ffn: float32 [2048], replicated, may hold values from 0.1 to 1.9
- w_gate: float32 [2048, 2816], P('fs', 'tp'), may hold values from -0.125 to 0.125
- scale_gate: float32 [2816], P('tp'), may hold values from 0.5 to 2
- w_up: float32 [2048, 2816], P('fs', 'tp'), may hold values from -0.125 to 0.125
- scale_up: float32 [2816], P('tp'), may hold values from 0.5 to 2
- w_down: float32 [2048, 2816], P('fs', 'tp'), may hold values from -0.109375 to 0.109375
- scale_down: float32 [2048], P('fs'), may hold values from 0.5 to 2
Outputs:
- layer_out: bfloat16 [2048, 2048], P(('rep', 'fs', 'tp'))
The draws below stay inside these ranges and needn't reach their ends.
All inputs are finite; a program needn't handle non-finite values.
Results may differ from the reference program's by a relative error of at most 0.015.
Values may be sent and summed in bfloat16 or wider, within the bound.
A program may use at most 64 MiB of HBM per device.

```python
import math
import jax
import jax.numpy as jnp
from jax import lax

D = 2048
HEADS = 8
DK = 256
DV = 256
FF = 2816
LEN = 128
BLK = 64
TOKENS = 2048
N_TP = 4


def block_scale(stream_key, shape, pieces, smallest, top_value):
    factor_of = 1.0
    for position, parts in pieces:
        heights = jax.random.uniform(jax.random.fold_in(jax.random.fold_in(stream_key, 6), position), (parts,), jnp.float32, smallest / len(pieces), top_value / len(pieces))
        factor_of = factor_of * jnp.repeat(jnp.exp(heights), shape[position] // parts).reshape((-1,) + (1,) * (len(shape) - 1 - position))
    return factor_of


def scatter_about(rng, extent, width, reach, cuts=(), kind=jnp.bfloat16):
    level = block_scale(rng, extent, cuts, -0.22, 0.18) if cuts else 1.0
    drawn = jax.random.normal(rng, extent, jnp.float32) * width * level
    return jnp.minimum(jnp.maximum(drawn, -reach), reach).astype(kind)


def setup_inputs(seed: int = 0) -> dict:
    arg_keys = jax.random.split(jax.random.key(seed), 16)
    return {
        "stream": scatter_about(arg_keys[0], (TOKENS, D), 1.0, 6.0, ((0, 8),)),
        "gain_mix": jnp.clip(1.0 + 0.18 * jax.random.normal(arg_keys[1], (D,), jnp.float32), 0.1, 1.9),
        "w_query": scatter_about(arg_keys[2], (D, HEADS * DK), D ** -0.5, 0.125, ((0, 4), (1, 4)), jnp.float32),
        "scale_query": jnp.clip(jnp.exp(math.log(2.0) - 1.3862944 * jax.random.uniform(arg_keys[3], (HEADS * DK,), jnp.float32) ** block_scale(arg_keys[3], (HEADS * DK,), ((0, 4),), -0.2, 0.2)), 0.5, 2.0),
        "w_key": scatter_about(arg_keys[4], (D, HEADS * DK), D ** -0.5, 0.125, ((0, 4), (1, 4)), jnp.float32),
        "scale_key": jnp.clip(jnp.exp(math.log(2.0) - 1.3862944 * jax.random.uniform(arg_keys[5], (HEADS * DK,), jnp.float32) ** block_scale(arg_keys[5], (HEADS * DK,), ((0, 4),), -0.2, 0.2)), 0.5, 2.0),
        "w_value": scatter_about(arg_keys[6], (D, HEADS * DV), D ** -0.5, 0.125, ((0, 4), (1, 4)), jnp.float32),
        "scale_value": jnp.clip(jnp.exp(math.log(2.0) - 1.3862944 * jax.random.uniform(arg_keys[7], (HEADS * DV,), jnp.float32) ** block_scale(arg_keys[7], (HEADS * DV,), ((0, 4),), -0.2, 0.2)), 0.5, 2.0),
        "gain_ffn": jnp.clip(1.0 + 0.18 * jax.random.normal(arg_keys[8], (D,), jnp.float32), 0.1, 1.9),
        "w_gate": scatter_about(arg_keys[9], (D, FF), D ** -0.5, 0.125, ((0, 4), (1, 4)), jnp.float32),
        "scale_gate": jnp.clip(jnp.exp(math.log(2.0) - 1.3862944 * jax.random.uniform(arg_keys[10], (FF,), jnp.float32) ** block_scale(arg_keys[10], (FF,), ((0, 4),), -0.2, 0.2)), 0.5, 2.0),
        "w_up": scatter_about(arg_keys[11], (D, FF), D ** -0.5, 0.125, ((0, 4), (1, 4)), jnp.float32),
        "scale_up": jnp.clip(jnp.exp(math.log(2.0) - 1.3862944 * jax.random.uniform(arg_keys[12], (FF,), jnp.float32) ** block_scale(arg_keys[12], (FF,), ((0, 4),), -0.2, 0.2)), 0.5, 2.0),
        "w_down": scatter_about(arg_keys[13], (D, FF), FF ** -0.5, 0.109375, ((0, 4), (1, 4)), jnp.float32),
        "scale_down": jnp.clip(jnp.exp(math.log(2.0) - 1.3862944 * jax.random.uniform(arg_keys[14], (D,), jnp.float32) ** block_scale(arg_keys[14], (D,), ((0, 4),), -0.2, 0.2)), 0.5, 2.0),
    }


EPS = 1e-06
THETA = 10000.0
HIGH = lax.Precision.HIGHEST

def rms_scale(values):
    return lax.rsqrt(lax.optimization_barrier(jnp.mean(values * values, axis=-1, keepdims=True)) + EPS)

def head_scale(values):
    return 1.0 / jnp.maximum(jnp.sqrt(lax.optimization_barrier(jnp.mean(values * values, axis=-1, keepdims=True))), 1.0)

def rotate(heads_data, positions):
    half = heads_data.shape[-1] // 2
    frequency = THETA ** (-(jnp.arange(half, dtype=jnp.float32) / half))
    angle = positions.astype(jnp.float32)[:, None, None] * frequency
    cosine = jnp.cos(angle)
    sine = jnp.sin(angle)
    first = heads_data[..., :half]
    second = heads_data[..., half:]
    return jnp.concatenate([first * cosine - second * sine, second * cosine + first * sine], axis=-1)

def retention_blocks(queries, keys, values, log_decay):
    total_rows, heads, key_width = queries.shape
    value_width = values.shape[-1]
    queries = queries.reshape((-1, LEN // BLK, BLK, heads, key_width))
    keys = keys.reshape((-1, LEN // BLK, BLK, heads, key_width))
    values = values.reshape((-1, LEN // BLK, BLK, heads, value_width))
    offsets = jnp.arange(BLK, dtype=jnp.float32)
    distance = offsets[:, None] - offsets[None, :]
    decay_mask = jnp.where(distance >= 0, jnp.exp(log_decay[:, None, None] * jnp.maximum(distance, 0.0)), 0.0)
    scores = jnp.einsum('snihd,snjhd->snhij', queries, keys, precision=HIGH) * decay_mask
    inner = jnp.einsum('snhij,snjhe->snihe', scores, values, precision=HIGH)
    query_decay = jnp.exp(log_decay[None, :] * (offsets[:, None] + 1.0))[:, :, None]
    key_decay = jnp.exp(log_decay[None, :] * (BLK - 1.0 - offsets[:, None]))[:, :, None]
    block_decay = jnp.exp(log_decay * BLK)[None, :, None, None]

    def advance(state, inputs):
        block_query, block_key, block_value = inputs
        carried = jnp.einsum('sihd,shde->sihe', block_query, state, precision=HIGH)
        state = state * block_decay + jnp.einsum('sjhd,sjhe->shde', block_key, block_value, precision=HIGH)
        return (state, carried)
    moved = (jnp.moveaxis(queries * query_decay, 1, 0), jnp.moveaxis(keys * key_decay, 1, 0), jnp.moveaxis(values, 1, 0))
    initial = jnp.zeros((queries.shape[0], heads, key_width, value_width), jnp.float32)
    _, carried = lax.scan(advance, initial, moved)
    return (inner + jnp.moveaxis(carried, 0, 1)).reshape(total_rows, heads, value_width)

def reference(stream, gain_mix, w_query, scale_query, w_key, scale_key, w_value, scale_value, gain_ffn, w_gate, scale_gate, w_up, scale_up, w_down, scale_down):
    stream_f = stream.astype(jnp.float32)
    normed = (stream_f * rms_scale(stream_f) * gain_mix).astype(jnp.bfloat16)

    def project(weight, scale):
        return (jnp.dot(normed, weight.astype(jnp.bfloat16), preferred_element_type=jnp.float32) * scale).astype(jnp.bfloat16)
    query = project(w_query, scale_query)
    key = project(w_key, scale_key)
    value = project(w_value, scale_value)
    total_rows = stream.shape[0]
    positions = jnp.arange(total_rows, dtype=jnp.int32) % LEN
    queries = rotate(query.astype(jnp.float32).reshape(total_rows, HEADS, DK), positions)
    keys = rotate(key.astype(jnp.float32).reshape(total_rows, HEADS, DK), positions) * DK ** (-0.5)
    values = value.astype(jnp.float32).reshape(total_rows, HEADS, DV)
    log_decay = jnp.log(1.0 - jnp.power(2.0, -5.0 - jnp.arange(HEADS, dtype=jnp.float32)))
    retained = retention_blocks(queries, keys, values, log_decay)
    mixed = (retained * head_scale(retained)).astype(jnp.bfloat16).reshape(total_rows, HEADS * DV)
    resid = stream_f + mixed.astype(jnp.float32)
    normed_ffn = (resid * rms_scale(resid) * gain_ffn).astype(jnp.bfloat16)
    gate = jnp.dot(normed_ffn, w_gate.astype(jnp.bfloat16), preferred_element_type=jnp.float32) * scale_gate
    upward = jnp.dot(normed_ffn, w_up.astype(jnp.bfloat16), preferred_element_type=jnp.float32) * scale_up
    hidden = (jax.nn.silu(gate) * upward).astype(jnp.bfloat16)
    down_rounded = w_down.astype(jnp.bfloat16)
    block_width = FF // N_TP
    channel_out = jnp.zeros((total_rows, D), jnp.float32)
    for number in range(N_TP):
        piece = hidden[:, number * block_width:(number + 1) * block_width]
        columns = down_rounded[:, number * block_width:(number + 1) * block_width]
        partial_sum = lax.dot_general(piece, columns, (((1,), (1,)), ((), ())), preferred_element_type=jnp.float32) * scale_down
        partial_sum = lax.optimization_barrier(partial_sum.astype(jnp.bfloat16))
        channel_out = channel_out + partial_sum.astype(jnp.float32)
    return (resid + channel_out).astype(jnp.bfloat16)
```

```python
import jax
import jax.numpy as jnp
from jax import lax
from jax.sharding import PartitionSpec as P

DK = 256
DV = 256
LEN = 128


EPS = 1e-06
THETA = 10000.0
HIGH = lax.Precision.HIGHEST


def rms_scale(values):
    return lax.rsqrt(jnp.mean(values * values, axis=-1, keepdims=True) + EPS)


def head_scale(values):
    return 1.0 / jnp.maximum(jnp.sqrt(jnp.mean(values * values, axis=-1, keepdims=True)), 1.0)


def rotate(heads_data, positions):
    half = heads_data.shape[-1] // 2
    frequency = THETA ** (-(jnp.arange(half, dtype=jnp.float32) / half))
    angle = positions.astype(jnp.float32)[:, None] * frequency
    cosine = jnp.cos(angle)
    sine = jnp.sin(angle)
    first = heads_data[..., :half]
    second = heads_data[..., half:]
    return jnp.concatenate(
        [first * cosine - second * sine, second * cosine + first * sine], axis=-1
    )


def retention(queries, keys, values, log_decay):
    offsets = jnp.arange(LEN, dtype=jnp.float32)
    distance = offsets[:, None] - offsets[None, :]
    decay = jnp.where(distance >= 0, jnp.exp(log_decay * jnp.maximum(distance, 0.0)), 0.0)
    queries, keys, values = (
        part.reshape(-1, LEN, part.shape[-1]) for part in (queries, keys, values)
    )
    scores = jnp.einsum("sid,sjd->sij", queries, keys, precision=HIGH) * decay
    retained = jnp.einsum("sij,sje->sie", scores, values, precision=HIGH)
    return retained.reshape(-1, values.shape[-1])


def split_rows(weight, mine):
    half = weight.shape[0] // 2
    return lax.dynamic_slice_in_dim(weight, mine * half, half, 0).astype(jnp.bfloat16)


def gathered(weight, mine):
    own = lax.all_gather(split_rows(weight, mine), "fs", axis=0, tiled=True)
    return own, lax.ppermute(own, "rep", [(0, 1), (1, 0)])


def column_halves(rows, shards_count, mine):
    width = rows.shape[1]
    parts = rows.reshape(rows.shape[0], shards_count, 2, width // (2 * shards_count))
    first = parts[:, :, 0].reshape(rows.shape[0], width // 2)
    second = parts[:, :, 1].reshape(rows.shape[0], width // 2)
    return jnp.where(mine == 0, first, second), jnp.where(mine == 0, second, first)


def dot(left, right):
    return jnp.dot(left, right, preferred_element_type=jnp.float32)


def dot_t(left, right):
    return lax.dot_general(left, right, (((1,), (1,)), ((), ())), preferred_element_type=jnp.float32)


def project(halves, weight_halves):
    return dot(halves[0], weight_halves[0]) + dot(halves[1], weight_halves[1])


def shards(
    stream,
    gain_mix,
    w_query,
    scale_query,
    w_key,
    scale_key,
    w_value,
    scale_value,
    gain_ffn,
    w_gate,
    scale_gate,
    w_up,
    scale_up,
    w_down,
    scale_down,
):
    group_rows = stream.shape[0]
    fs_count = lax.axis_size("fs")
    paired = lax.axis_size("rep") == 2
    mine = lax.axis_index("rep")
    stream_f = stream.astype(jnp.float32)
    normed = (stream_f * rms_scale(stream_f) * gain_mix).astype(jnp.bfloat16)
    down_scale = lax.all_gather(scale_down, "fs", axis=0, tiled=True)
    if paired:
        query_w, key_w, value_w, gate_w, up_w, down_w = (
            gathered(w, mine) for w in (w_query, w_key, w_value, w_gate, w_up, w_down)
        )
        spread = lambda rows: column_halves(rows, fs_count, mine)
        times = project
    else:
        query_w, key_w, value_w, gate_w, up_w, down_w = (
            lax.all_gather(w.astype(jnp.bfloat16), "fs", axis=0, tiled=True)
            for w in (w_query, w_key, w_value, w_gate, w_up, w_down)
        )
        spread = lambda rows: rows
        times = dot
    normed = spread(normed)
    query = (times(normed, query_w) * scale_query).astype(jnp.bfloat16)
    key = (times(normed, key_w) * scale_key).astype(jnp.bfloat16)
    value = (times(normed, value_w) * scale_value).astype(jnp.bfloat16)
    local_heads = query.shape[1] // DK
    positions = jnp.arange(group_rows, dtype=jnp.int32) % LEN
    mixed = []
    for head in range(local_heads):
        columns = slice(head * DK, (head + 1) * DK)
        queries = rotate(query[:, columns].astype(jnp.float32), positions)
        keys = rotate(key[:, columns].astype(jnp.float32), positions) * DK ** (-0.5)
        values = value[:, head * DV : (head + 1) * DV].astype(jnp.float32)
        head_id = (lax.axis_index("tp") * local_heads + head).astype(jnp.float32)
        log_decay = jnp.log(1.0 - jnp.power(2.0, -5.0 - head_id))
        retained = retention(queries, keys, values, log_decay)
        mixed.append((retained * head_scale(retained)).astype(jnp.bfloat16))
    mixed = jnp.concatenate(mixed, axis=1)
    arrived = lax.all_to_all(mixed, "tp", split_axis=0, concat_axis=1, tiled=True)
    share = arrived.shape[0]
    own_rows = lax.dynamic_slice_in_dim(stream, lax.axis_index("tp") * share, share, 0)
    resid = own_rows.astype(jnp.float32) + arrived.astype(jnp.float32)
    normed_ffn = (resid * rms_scale(resid) * gain_ffn).astype(jnp.bfloat16)
    piece = spread(lax.all_gather(normed_ffn, "tp", axis=0, tiled=True))
    gate = times(piece, gate_w) * scale_gate
    upward = times(piece, up_w) * scale_up
    hidden = (jax.nn.silu(gate) * upward).astype(jnp.bfloat16)
    if paired:
        own, other = (dot_t(hidden, w).reshape(group_rows, fs_count, 1, -1) for w in down_w)
        first = jnp.where(mine == 0, own, other)
        second = jnp.where(mine == 0, other, own)
        partial_sum = jnp.concatenate([first, second], axis=2).reshape(group_rows, -1)
    else:
        partial_sum = dot_t(hidden, down_w)
    partial_sum = (partial_sum * down_scale).astype(jnp.bfloat16)
    partial_sum = partial_sum.reshape(-1, share, partial_sum.shape[1])
    pieces = lax.all_to_all(partial_sum, "tp", split_axis=0, concat_axis=0)
    channel_out = jnp.sum(pieces.astype(jnp.float32), axis=0)
    return (resid + channel_out).astype(jnp.bfloat16)


def solution(mesh):
    placed = (
        P(("rep", "fs"), None),
        P(),
        P("fs", "tp"),
        P("tp"),
        P("fs", "tp"),
        P("tp"),
        P("fs", "tp"),
        P("tp"),
        P(),
        P("fs", "tp"),
        P("tp"),
        P("fs", "tp"),
        P("tp"),
        P("fs", "tp"),
        P("fs"),
    )
    return jax.shard_map(
        shards, mesh=mesh, in_specs=placed, out_specs=P(("rep", "fs", "tp"), None), check_vma=False
    )
```

```python
import jax
import jax.numpy as jnp
from jax import lax
from jax.sharding import PartitionSpec as P

DK = 256
DV = 256
LEN = 128


EPS = 1e-06
THETA = 10000.0
HIGH = lax.Precision.HIGHEST


def rms_scale(values):
    return lax.rsqrt(jnp.mean(values * values, axis=-1, keepdims=True) + EPS)


def head_scale(values):
    return 1.0 / jnp.maximum(jnp.sqrt(jnp.mean(values * values, axis=-1, keepdims=True)), 1.0)


def rotate(heads_data, positions):
    half = heads_data.shape[-1] // 2
    frequency = THETA ** (-(jnp.arange(half, dtype=jnp.float32) / half))
    angle = positions.astype(jnp.float32)[:, None] * frequency
    cosine = jnp.cos(angle)
    sine = jnp.sin(angle)
    first = heads_data[..., :half]
    second = heads_data[..., half:]
    return jnp.concatenate(
        [first * cosine - second * sine, second * cosine + first * sine], axis=-1
    )


def retention(queries, keys, values, log_decay):
    offsets = jnp.arange(LEN, dtype=jnp.float32)
    distance = offsets[:, None] - offsets[None, :]
    decay = jnp.where(distance >= 0, jnp.exp(log_decay * jnp.maximum(distance, 0.0)), 0.0)
    queries, keys, values = (
        part.reshape(-1, LEN, part.shape[-1]) for part in (queries, keys, values)
    )
    scores = jnp.einsum("sid,sjd->sij", queries, keys, precision=HIGH) * decay
    retained = jnp.einsum("sij,sje->sie", scores, values, precision=HIGH)
    return retained.reshape(-1, values.shape[-1])


def dot(left, right):
    return jnp.dot(left, right, preferred_element_type=jnp.float32)


def dot_t(left, right):
    return lax.dot_general(left, right, (((1,), (1,)), ((), ())), preferred_element_type=jnp.float32)


def line_steps(block, count):
    below, above = [block], [block]
    for step in range(1, count):
        below.append(
            lax.ppermute(below[-1], "fs", [(i, i + 1) for i in range(step - 1, count - 1)])
        )
        above.append(
            lax.ppermute(above[-1], "fs", [(i, i - 1) for i in range(1, count - step + 1)])
        )
    return below, above


def line_gather(weight, mine, place):
    half = weight.shape[0] // 2
    below, above = line_steps(lax.dynamic_slice_in_dim(weight, mine * half, half, 0), 4)
    outer = (place == 0) | (place == 3)
    slots = (
        jnp.where(place == 0, above[1], below[1]),
        jnp.where(place < 2, above[2], below[2]),
        jnp.where(outer, jnp.where(place == 0, above[3], below[3]), above[1]),
    )
    return [(slot, lax.ppermute(slot, "rep", [(0, 1), (1, 0)])) for slot in slots]


def line_sources(place):
    outer = (place == 0) | (place == 3)
    return (
        jnp.where(place == 0, 1, place - 1),
        jnp.where(place < 2, place + 2, place - 2),
        jnp.where(outer, 3 - place, place + 1),
    )


def columns_of(rows, start, width):
    return lax.dynamic_slice_in_dim(rows, start, width, 1)


def line_project(rows, own, slots, mine, place):
    width = own.shape[0]
    half = width // 2
    total = dot(columns_of(rows, place * width, width), own)
    for source, (near, far) in zip(line_sources(place), slots):
        total += dot(columns_of(rows, source * width + mine * half, half), near)
        total += dot(columns_of(rows, source * width + (1 - mine) * half, half), far)
    return total


def line_down(hidden, own, slots, scales, mine, place):
    width = own.shape[0]
    half = width // 2
    blocks, starts = [dot_t(hidden, own)], [place * width]
    for source, (near, far) in zip(line_sources(place), slots):
        for block, side in ((near, mine), (far, 1 - mine)):
            blocks.append(dot_t(hidden, block))
            starts.append(source * width + side * half)
    blocks = [
        (block * lax.dynamic_slice_in_dim(scales, start, block.shape[1], 0)).astype(jnp.bfloat16)
        for block, start in zip(blocks, starts)
    ]
    return blocks, starts


def summed_over_tp(partial_sum, share):
    partial_sum = partial_sum.reshape(-1, share, partial_sum.shape[1])
    pieces = lax.all_to_all(partial_sum, "tp", split_axis=0, concat_axis=0)
    return jnp.sum(pieces.astype(jnp.float32), axis=0)


def shards(
    stream,
    gain_mix,
    w_query,
    scale_query,
    w_key,
    scale_key,
    w_value,
    scale_value,
    gain_ffn,
    w_gate,
    scale_gate,
    w_up,
    scale_up,
    w_down,
    scale_down,
):
    group_rows = stream.shape[0]
    mine = lax.axis_index("rep")
    place = lax.axis_index("fs")
    on_line = lax.axis_size("rep") == 2 and lax.axis_size("fs") == 4
    stream_f = stream.astype(jnp.float32)
    normed = (stream_f * rms_scale(stream_f) * gain_mix).astype(jnp.bfloat16)
    down_scale = lax.all_gather(scale_down, "fs", axis=0, tiled=True)
    mix_w = jnp.concatenate([w.astype(jnp.bfloat16) for w in (w_query, w_key, w_value)], axis=1)
    up_w = jnp.concatenate([w.astype(jnp.bfloat16) for w in (w_gate, w_up)], axis=1)
    down_w = w_down.astype(jnp.bfloat16)
    if on_line:
        mix_slots, up_slots, down_slots = (line_gather(w, mine, place) for w in (mix_w, up_w, down_w))
        mix_acc = line_project(normed, mix_w, mix_slots, mine, place)
    else:
        mix_acc = dot(normed, lax.all_gather(mix_w, "fs", axis=0, tiled=True))
    mix_scale = jnp.concatenate([scale_query, scale_key, scale_value])
    query, key, value = jnp.split(
        (mix_acc * mix_scale).astype(jnp.bfloat16),
        [w_query.shape[1], w_query.shape[1] + w_key.shape[1]],
        axis=1,
    )
    local_heads = query.shape[1] // DK
    positions = jnp.arange(group_rows, dtype=jnp.int32) % LEN
    mixed = []
    for head in range(local_heads):
        columns = slice(head * DK, (head + 1) * DK)
        queries = rotate(query[:, columns].astype(jnp.float32), positions)
        keys = rotate(key[:, columns].astype(jnp.float32), positions) * DK ** (-0.5)
        values = value[:, head * DV : (head + 1) * DV].astype(jnp.float32)
        head_id = (lax.axis_index("tp") * local_heads + head).astype(jnp.float32)
        log_decay = jnp.log(1.0 - jnp.power(2.0, -5.0 - head_id))
        retained = retention(queries, keys, values, log_decay)
        mixed.append((retained * head_scale(retained)).astype(jnp.bfloat16))
    mixed = jnp.concatenate(mixed, axis=1)
    arrived = lax.all_to_all(mixed, "tp", split_axis=0, concat_axis=1, tiled=True)
    share = arrived.shape[0]
    own_rows = lax.dynamic_slice_in_dim(stream, lax.axis_index("tp") * share, share, 0)
    resid = own_rows.astype(jnp.float32) + arrived.astype(jnp.float32)
    normed_ffn = (resid * rms_scale(resid) * gain_ffn).astype(jnp.bfloat16)
    piece = lax.all_gather(normed_ffn, "tp", axis=0, tiled=True)
    if on_line:
        up_acc = line_project(piece, up_w, up_slots, mine, place)
    else:
        up_acc = dot(piece, lax.all_gather(up_w, "fs", axis=0, tiled=True))
    units = w_gate.shape[1]
    gate = up_acc[:, :units] * scale_gate
    upward = up_acc[:, units:] * scale_up
    hidden = (jax.nn.silu(gate) * upward).astype(jnp.bfloat16)
    if on_line:
        blocks, starts = line_down(hidden, down_w, down_slots, down_scale, mine, place)
        sums = summed_over_tp(jnp.concatenate(blocks, axis=1), share)
        channel_out = jnp.zeros_like(resid)
        offset = 0
        for block, start in zip(blocks, starts):
            width = block.shape[1]
            channel_out = lax.dynamic_update_slice_in_dim(
                channel_out, sums[:, offset : offset + width], start, 1
            )
            offset += width
    else:
        whole = dot_t(hidden, lax.all_gather(down_w, "fs", axis=0, tiled=True))
        channel_out = summed_over_tp((whole * down_scale).astype(jnp.bfloat16), share)
    return (resid + channel_out).astype(jnp.bfloat16)


def solution(mesh):
    placed = (
        P(("rep", "fs"), None),
        P(),
        P("fs", "tp"),
        P("tp"),
        P("fs", "tp"),
        P("tp"),
        P("fs", "tp"),
        P("tp"),
        P(),
        P("fs", "tp"),
        P("tp"),
        P("fs", "tp"),
        P("tp"),
        P("fs", "tp"),
        P("fs"),
    )
    return jax.shard_map(
        shards, mesh=mesh, in_specs=placed, out_specs=P(("rep", "fs", "tp"), None), check_vma=False
    )
```

```python
import jax
import jax.numpy as jnp
from jax import lax
from jax.experimental import pallas as pl
from jax.experimental.pallas import tpu as pltpu
from jax.sharding import PartitionSpec as P

DK = 256
DV = 256
LEN = 128


EPS = 1e-06
THETA = 10000.0
HIGH = lax.Precision.HIGHEST


def rms_scale(values):
    return lax.rsqrt(jnp.mean(values * values, axis=-1, keepdims=True) + EPS)


def head_scale(values):
    return 1.0 / jnp.maximum(jnp.sqrt(jnp.mean(values * values, axis=-1, keepdims=True)), 1.0)


def rotate(heads_data, positions):
    half = heads_data.shape[-1] // 2
    frequency = THETA ** (-(jnp.arange(half, dtype=jnp.float32) / half))
    angle = positions.astype(jnp.float32)[:, None] * frequency
    cosine = jnp.cos(angle)
    sine = jnp.sin(angle)
    first = heads_data[..., :half]
    second = heads_data[..., half:]
    return jnp.concatenate(
        [first * cosine - second * sine, second * cosine + first * sine], axis=-1
    )


def retention(queries, keys, values, log_decay):
    offsets = jnp.arange(LEN, dtype=jnp.float32)
    distance = offsets[:, None] - offsets[None, :]
    decay = jnp.where(distance >= 0, jnp.exp(log_decay * jnp.maximum(distance, 0.0)), 0.0)
    queries, keys, values = (
        part.reshape(-1, LEN, part.shape[-1]) for part in (queries, keys, values)
    )
    scores = jnp.einsum("sid,sjd->sij", queries, keys, precision=HIGH) * decay
    retained = jnp.einsum("sij,sje->sie", scores, values, precision=HIGH)
    return retained.reshape(-1, values.shape[-1])


def dot(left, right):
    return jnp.dot(left, right, preferred_element_type=jnp.float32)


def dot_t(left, right):
    return lax.dot_general(left, right, (((1,), (1,)), ((), ())), preferred_element_type=jnp.float32)


def line_steps(block, count):
    below, above = [block], [block]
    for step in range(1, count):
        below.append(
            lax.ppermute(below[-1], "fs", [(i, i + 1) for i in range(step - 1, count - 1)])
        )
        above.append(
            lax.ppermute(above[-1], "fs", [(i, i - 1) for i in range(1, count - step + 1)])
        )
    return below, above


def line_gather(weight, mine, place):
    half = weight.shape[0] // 2
    below, above = line_steps(lax.dynamic_slice_in_dim(weight, mine * half, half, 0), 4)
    outer = (place == 0) | (place == 3)
    slots = (
        jnp.where(place == 0, above[1], below[1]),
        jnp.where(place < 2, above[2], below[2]),
        jnp.where(outer, jnp.where(place == 0, above[3], below[3]), above[1]),
    )
    return [(slot, lax.ppermute(slot, "rep", [(0, 1), (1, 0)])) for slot in slots]


def line_sources(place):
    outer = (place == 0) | (place == 3)
    return (
        jnp.where(place == 0, 1, place - 1),
        jnp.where(place < 2, place + 2, place - 2),
        jnp.where(outer, 3 - place, place + 1),
    )


CHUNKS = 4
MESH = pl.DeviceIdType.MESH


def gather_kernel(half_ref, scale_ref, near, far, scales, down_send, down_recv, up_send, up_recv,
                  side_send, side_recv, scale_send, scale_recv):
    place, mine = lax.axis_index("fs"), lax.axis_index("rep")
    count = 4
    barrier = pltpu.get_barrier_semaphore()
    for step in range(1, count):
        pl.semaphore_signal(
            barrier, inc=1, device_id={"fs": lax.rem(place + step, count)}, device_id_type=MESH
        )
    pl.semaphore_signal(barrier, inc=1, device_id={"rep": 1 - mine}, device_id_type=MESH)
    pl.semaphore_wait(barrier, count)
    height = half_ref.shape[0] // CHUNKS

    def hop(upward, step, chunk):
        rows = pl.ds(chunk * height, height)
        source = place - (step - 1) if upward else place + (step - 1)
        block = half_ref.at[rows] if step == 1 else near.at[source, rows]
        send, recv = (up_send, up_recv) if upward else (down_send, down_recv)
        return pltpu.make_async_remote_copy(
            src_ref=block,
            dst_ref=near.at[source, rows],
            send_sem=send.at[step - 1, chunk],
            recv_sem=recv.at[step - 1, chunk],
            device_id={"fs": place + 1 if upward else place - 1},
            device_id_type=MESH,
        )

    def arriving(upward, step, chunk):
        rows = pl.ds(chunk * height, height)
        source = place - step if upward else place + step
        send, recv = (up_send, up_recv) if upward else (down_send, down_recv)
        return pltpu.make_async_remote_copy(
            src_ref=near.at[source, rows],
            dst_ref=near.at[source, rows],
            send_sem=send.at[step - 1, chunk],
            recv_sem=recv.at[step - 1, chunk],
            device_id={"fs": place - 1 if upward else place + 1},
            device_id_type=MESH,
        )

    def over(upward, step, chunk):
        rows = pl.ds(chunk * height, height)
        source = place - step if upward else place + step
        way = 0 if upward else 1
        return pltpu.make_async_remote_copy(
            src_ref=near.at[source, rows],
            dst_ref=far.at[source, rows],
            send_sem=side_send.at[way, step - 1, chunk],
            recv_sem=side_recv.at[way, step - 1, chunk],
            device_id={"rep": 1 - mine},
            device_id_type=MESH,
        )

    def scale_copy(step):
        return pltpu.make_async_remote_copy(
            src_ref=scale_ref,
            dst_ref=scales.at[place],
            send_sem=scale_send.at[step - 1],
            recv_sem=scale_recv.at[step - 1],
            device_id={"fs": lax.rem(place + step, count)},
            device_id_type=MESH,
        )

    def sends(upward, step):
        if upward:
            return (place >= step - 1) & (place < count - 1)
        return (place <= count - step) & (place > 0)

    def receives(upward, step):
        return place >= step if upward else place < count - step

    for chunk in range(CHUNKS):
        for upward in (True, False):
            @pl.when(sends(upward, 1))
            def _():
                hop(upward, 1, chunk).start()
    for step in range(1, count):
        scale_copy(step).start()
    for step in range(1, count):
        for chunk in range(CHUNKS):
            for upward in (True, False):
                @pl.when(receives(upward, step))
                def _():
                    arriving(upward, step, chunk).wait_recv()
                    over(upward, step, chunk).start()

                if step < count - 1:
                    @pl.when(sends(upward, step + 1))
                    def _():
                        hop(upward, step + 1, chunk).start()
    for step in range(1, count):
        scale_copy(step).wait()
        for chunk in range(CHUNKS):
            for upward in (True, False):
                @pl.when(receives(upward, step))
                def _():
                    over(upward, step, chunk).wait()

                @pl.when(sends(upward, step))
                def _():
                    hop(upward, step, chunk).wait_send()


def kernel_gather(half, scale, collective_id):
    shape = jax.ShapeDtypeStruct((4, *half.shape), half.dtype)
    steps = pltpu.SemaphoreType.DMA((3, CHUNKS))
    sides = pltpu.SemaphoreType.DMA((2, 3, CHUNKS))
    few = pltpu.SemaphoreType.DMA((3,))
    anywhere = pl.BlockSpec(memory_space=pl.ANY)
    return pl.pallas_call(
        gather_kernel,
        out_shape=(shape, shape, jax.ShapeDtypeStruct((4, *scale.shape), scale.dtype)),
        in_specs=[anywhere] * 2,
        out_specs=(anywhere,) * 3,
        scratch_shapes=[steps, steps, steps, steps, sides, sides, few, few],
        compiler_params=pltpu.CompilerParams(collective_id=collective_id, has_side_effects=True),
    )(half, scale)


def own_half(weight, mine):
    half = weight.shape[0] // 2
    return lax.dynamic_slice_in_dim(weight, mine * half, half, 0)


def arrived_slots(near, far, place):
    pick = lambda blocks, source: lax.dynamic_index_in_dim(blocks, source, 0, keepdims=False)
    return [(pick(near, source), pick(far, source)) for source in line_sources(place)]


def gather_over_tp(block):
    far = lax.ppermute(block, "tp", [(j, j ^ 2) for j in range(4)])
    both = jnp.stack([block, far])
    other = lax.ppermute(both, "tp", [(j, j ^ 1) for j in range(4)])
    return jnp.concatenate([both, other])


def in_tp_order(blocks):
    here = lax.axis_index("tp")
    order = [here ^ j for j in range(4)]
    spot = lambda d: jnp.where((d == 0) | (d == 3), d, 3 - d)
    return jnp.concatenate(
        [lax.dynamic_index_in_dim(blocks, spot(d), 0, keepdims=True) for d in order]
    )


def columns_of(rows, start, width):
    return lax.dynamic_slice_in_dim(rows, start, width, 1)


def line_project(rows, own, slots, mine, place):
    width = own.shape[0]
    half = width // 2
    total = dot(columns_of(rows, place * width, width), own)
    for source, (near, far) in zip(line_sources(place), slots):
        total += dot(columns_of(rows, source * width + mine * half, half), near)
        total += dot(columns_of(rows, source * width + (1 - mine) * half, half), far)
    return total


def line_down(hidden, own, slots, scales, mine, place):
    width = own.shape[0]
    half = width // 2
    blocks, starts = [dot_t(hidden, own)], [place * width]
    for source, (near, far) in zip(line_sources(place), slots):
        for block, side in ((near, mine), (far, 1 - mine)):
            blocks.append(dot_t(hidden, block))
            starts.append(source * width + side * half)
    blocks = [
        (block * lax.dynamic_slice_in_dim(scales, start, block.shape[1], 0)).astype(jnp.bfloat16)
        for block, start in zip(blocks, starts)
    ]
    return blocks, starts


def summed_over_tp(partial_sum, share):
    partial_sum = partial_sum.reshape(-1, share, partial_sum.shape[1])
    pieces = lax.all_to_all(partial_sum, "tp", split_axis=0, concat_axis=0)
    return jnp.sum(pieces.astype(jnp.float32), axis=0)


def shards(
    stream,
    gain_mix,
    w_query,
    scale_query,
    w_key,
    scale_key,
    w_value,
    scale_value,
    gain_ffn,
    w_gate,
    scale_gate,
    w_up,
    scale_up,
    w_down,
    scale_down,
):
    group_rows = stream.shape[0]
    mine = lax.axis_index("rep")
    place = lax.axis_index("fs")
    on_line = lax.axis_size("rep") == 2 and lax.axis_size("fs") == 4
    stream_f = stream.astype(jnp.float32)
    normed = (stream_f * rms_scale(stream_f) * gain_mix).astype(jnp.bfloat16)
    mix_w = jnp.concatenate([w.astype(jnp.bfloat16) for w in (w_query, w_key, w_value)], axis=1)
    up_w = jnp.concatenate([w.astype(jnp.bfloat16) for w in (w_gate, w_up)], axis=1)
    down_w = w_down.astype(jnp.bfloat16)
    if on_line:
        near, far, scales = kernel_gather(own_half(mix_w, mine), scale_down[None, :], 0)
        scales = lax.dynamic_update_slice(scales, scale_down[None, None, :], (place, 0, 0))
        down_scale = scales.reshape(-1)
        mix_acc = line_project(normed, mix_w, arrived_slots(near, far, place), mine, place)
        down_w, far = lax.optimization_barrier((down_w, far))
        down_slots = line_gather(down_w, mine, place)
    else:
        down_scale = lax.all_gather(scale_down, "fs", axis=0, tiled=True)
        mix_acc = dot(normed, lax.all_gather(mix_w, "fs", axis=0, tiled=True))
    mix_scale = jnp.concatenate([scale_query, scale_key, scale_value])
    query, key, value = jnp.split(
        (mix_acc * mix_scale).astype(jnp.bfloat16),
        [w_query.shape[1], w_query.shape[1] + w_key.shape[1]],
        axis=1,
    )
    local_heads = query.shape[1] // DK
    positions = jnp.arange(group_rows, dtype=jnp.int32) % LEN
    mixed = []
    for head in range(local_heads):
        columns = slice(head * DK, (head + 1) * DK)
        queries = rotate(query[:, columns].astype(jnp.float32), positions)
        keys = rotate(key[:, columns].astype(jnp.float32), positions) * DK ** (-0.5)
        values = value[:, head * DV : (head + 1) * DV].astype(jnp.float32)
        head_id = (lax.axis_index("tp") * local_heads + head).astype(jnp.float32)
        log_decay = jnp.log(1.0 - jnp.power(2.0, -5.0 - head_id))
        retained = retention(queries, keys, values, log_decay)
        mixed.append((retained * head_scale(retained)).astype(jnp.bfloat16))
    mixed = jnp.concatenate(mixed, axis=1)
    arrived = lax.all_to_all(mixed, "tp", split_axis=0, concat_axis=1, tiled=True)
    share = arrived.shape[0]
    own_rows = lax.dynamic_slice_in_dim(stream, lax.axis_index("tp") * share, share, 0)
    resid = own_rows.astype(jnp.float32) + arrived.astype(jnp.float32)
    normed_ffn = (resid * rms_scale(resid) * gain_ffn).astype(jnp.bfloat16)
    four = on_line and lax.axis_size("tp") == 4
    if four:
        piece = gather_over_tp(normed_ffn).reshape(group_rows, -1)
    else:
        piece = lax.all_gather(normed_ffn, "tp", axis=0, tiled=True)
    if on_line:
        half, piece, *flat = lax.optimization_barrier(
            (own_half(up_w, mine), piece, *(b for pair in down_slots for b in pair))
        )
        down_slots = list(zip(flat[::2], flat[1::2]))
        near, far, _ = kernel_gather(half, scale_down[None, :], 1)
        up_acc = line_project(piece, up_w, arrived_slots(near, far, place), mine, place)
    else:
        up_acc = dot(piece, lax.all_gather(up_w, "fs", axis=0, tiled=True))
    units = w_gate.shape[1]
    gate = up_acc[:, :units] * scale_gate
    upward = up_acc[:, units:] * scale_up
    hidden = (jax.nn.silu(gate) * upward).astype(jnp.bfloat16)
    if four:
        hidden = in_tp_order(hidden.reshape(4, share, units)).reshape(group_rows, units)
    if on_line:
        blocks, starts = line_down(hidden, down_w, down_slots, down_scale, mine, place)
        sums = summed_over_tp(jnp.concatenate(blocks, axis=1), share)
        channel_out = jnp.zeros_like(resid)
        offset = 0
        for block, start in zip(blocks, starts):
            width = block.shape[1]
            channel_out = lax.dynamic_update_slice_in_dim(
                channel_out, sums[:, offset : offset + width], start, 1
            )
            offset += width
    else:
        whole = dot_t(hidden, lax.all_gather(down_w, "fs", axis=0, tiled=True))
        channel_out = summed_over_tp((whole * down_scale).astype(jnp.bfloat16), share)
    return (resid + channel_out).astype(jnp.bfloat16)


def solution(mesh):
    placed = (
        P(("rep", "fs"), None),
        P(),
        P("fs", "tp"),
        P("tp"),
        P("fs", "tp"),
        P("tp"),
        P("fs", "tp"),
        P("tp"),
        P(),
        P("fs", "tp"),
        P("tp"),
        P("fs", "tp"),
        P("tp"),
        P("fs", "tp"),
        P("fs"),
    )
    return jax.shard_map(
        shards, mesh=mesh, in_specs=placed, out_specs=P(("rep", "fs", "tp"), None), check_vma=False
    )
```

```python
import jax
import jax.numpy as jnp
from jax import lax
from jax.experimental import pallas as pl
from jax.experimental.pallas import tpu as pltpu
from jax.sharding import PartitionSpec as P

DK = 256
DV = 256
LEN = 128


EPS = 1e-06
THETA = 10000.0
HIGH = lax.Precision.HIGHEST


def rms_scale(values):
    return lax.rsqrt(jnp.mean(values * values, axis=-1, keepdims=True) + EPS)


def head_scale(values):
    return 1.0 / jnp.maximum(jnp.sqrt(jnp.mean(values * values, axis=-1, keepdims=True)), 1.0)


def rotate(heads_data, positions):
    half = heads_data.shape[-1] // 2
    frequency = THETA ** (-(jnp.arange(half, dtype=jnp.float32) / half))
    angle = positions.astype(jnp.float32)[:, None] * frequency
    cosine = jnp.cos(angle)
    sine = jnp.sin(angle)
    first = heads_data[..., :half]
    second = heads_data[..., half:]
    return jnp.concatenate(
        [first * cosine - second * sine, second * cosine + first * sine], axis=-1
    )


def retention(queries, keys, values, log_decay):
    offsets = jnp.arange(LEN, dtype=jnp.float32)
    distance = offsets[:, None] - offsets[None, :]
    decay = jnp.where(distance >= 0, jnp.exp(log_decay * jnp.maximum(distance, 0.0)), 0.0)
    queries, keys, values = (
        part.reshape(-1, LEN, part.shape[-1]) for part in (queries, keys, values)
    )
    scores = jnp.einsum("sid,sjd->sij", queries, keys, precision=HIGH) * decay
    retained = jnp.einsum("sij,sje->sie", scores, values, precision=HIGH)
    return retained.reshape(-1, values.shape[-1])


def dot(left, right):
    return jnp.dot(left, right, preferred_element_type=jnp.float32)


def dot_t(left, right):
    return lax.dot_general(left, right, (((1,), (1,)), ((), ())), preferred_element_type=jnp.float32)


def line_sources(place):
    outer = (place == 0) | (place == 3)
    return (
        jnp.where(place == 0, 1, place - 1),
        jnp.where(place < 2, place + 2, place - 2),
        jnp.where(outer, 3 - place, place + 1),
    )


CHUNKS = 4
MESH = pl.DeviceIdType.MESH


class Line:
    count = 4

    def __init__(self, halves, nears, fars, sems):
        self.halves, self.nears, self.fars, self.sems = halves, nears, fars, sems
        self.place, self.mine = lax.axis_index("fs"), lax.axis_index("rep")

    def part(self, group, chunk):
        height = self.halves[group].shape[0] // CHUNKS
        return pl.ds(chunk * height, height)

    def source(self, upward, step):
        return self.place - step if upward else self.place + step

    def hop(self, group, upward, step, chunk):
        rows, source = self.part(group, chunk), self.source(upward, step - 1)
        near = self.nears[group]
        block = self.halves[group].at[rows] if step == 1 else near.at[source, rows]
        way = 0 if upward else 1
        return pltpu.make_async_remote_copy(
            src_ref=block,
            dst_ref=near.at[source, rows],
            send_sem=self.sems[0].at[group, way, step - 1, chunk],
            recv_sem=self.sems[1].at[group, way, step - 1, chunk],
            device_id={"fs": self.place + 1 if upward else self.place - 1},
            device_id_type=MESH,
        )

    def passed(self, group, upward, step, chunk, over):
        rows, source = self.part(group, chunk), self.source(upward, step)
        near, first = self.nears[group], 2 if over else 0
        way = 0 if upward else 1
        return pltpu.make_async_remote_copy(
            src_ref=near.at[source, rows],
            dst_ref=(self.fars if over else self.nears)[group].at[source, rows],
            send_sem=self.sems[first].at[group, way, step - 1, chunk],
            recv_sem=self.sems[first + 1].at[group, way, step - 1, chunk],
            device_id={"rep": 1 - self.mine},
            device_id_type=MESH,
        )

    def sends(self, upward, step):
        if upward:
            return (self.place >= step - 1) & (self.place < self.count - 1)
        return (self.place <= self.count - step) & (self.place > 0)

    def receives(self, upward, step):
        return self.place >= step if upward else self.place < self.count - step

    def begin(self, group):
        for chunk in range(CHUNKS):
            for upward in (True, False):
                @pl.when(self.sends(upward, 1))
                def _():
                    self.hop(group, upward, 1, chunk).start()

    def pump(self, group, step):
        for chunk in range(CHUNKS):
            for upward in (True, False):
                @pl.when(self.receives(upward, step))
                def _():
                    self.passed(group, upward, step, chunk, False).wait_recv()
                    self.passed(group, upward, step, chunk, True).start()

                if step < self.count - 1:
                    @pl.when(self.sends(upward, step + 1))
                    def _():
                        self.hop(group, upward, step + 1, chunk).start()

    def finish(self, group):
        for step in range(1, self.count):
            for chunk in range(CHUNKS):
                for upward in (True, False):
                    @pl.when(self.receives(upward, step))
                    def _():
                        self.passed(group, upward, step, chunk, True).wait()

                    @pl.when(self.sends(upward, step))
                    def _():
                        self.hop(group, upward, step, chunk).wait_send()


def exchange(axis, count, source, target, sends, recvs):
    me = lax.axis_index(axis)
    copies = []
    for step in range(1, count):
        peer = lax.rem(me + step, count)
        copies.append(
            pltpu.make_async_remote_copy(
                src_ref=source(peer),
                dst_ref=target(me),
                send_sem=sends.at[step - 1],
                recv_sem=recvs.at[step - 1],
                device_id={axis: peer},
                device_id_type=MESH,
            )
        )
    return copies


def greet(peers):
    barrier = pltpu.get_barrier_semaphore()
    total = 0
    for axis, count in peers:
        me = lax.axis_index(axis)
        for step in range(1, count):
            peer = lax.rem(me + step, count)
            pl.semaphore_signal(barrier, inc=1, device_id={axis: peer}, device_id_type=MESH)
            total += 1
    pl.semaphore_wait(barrier, total)


def mix_kernel(half, scale, near, far, scales, s0, s1, s2, s3, scale_send, scale_recv):
    greet((("fs", 4), ("rep", 2)))
    line = Line([half], [near], [far], (s0, s1, s2, s3))
    line.begin(0)
    copies = exchange("fs", 4, lambda _: scale, lambda me: scales.at[me], scale_send, scale_recv)
    for copy in copies:
        copy.start()
    for step in range(1, 4):
        line.pump(0, step)
    for copy in copies:
        copy.wait()
    line.finish(0)


def ffn_kernel(half_up, half_down, mixed, rows, gain, near_up, far_up, near_down, far_down, piece,
               resid, s0, s1, s2, s3, arrived, normed, mix_send, mix_recv, row_send, row_recv,
               local):
    count, _, width = mixed.shape
    greet((("fs", 4), ("rep", 2), ("tp", count)))
    me = lax.axis_index("tp")
    line = Line([half_up, half_down], [near_up, near_down], [far_up, far_down], (s0, s1, s2, s3))
    line.begin(0)
    to_owners = exchange(
        "tp", count, lambda peer: mixed.at[peer], lambda me: arrived.at[me], mix_send, mix_recv
    )
    for copy in to_owners:
        copy.start()
    kept = pltpu.make_async_copy(mixed.at[me], arrived.at[me], local.at[0])
    kept.start()
    line.begin(1)
    for copy in to_owners:
        copy.wait()
    kept.wait()
    squares = 0.0
    for block in range(count):
        columns = slice(block * width, (block + 1) * width)
        values = rows[:, columns].astype(jnp.float32) + arrived[block].astype(jnp.float32)
        resid[:, columns] = values
        squares += jnp.sum(values * values, axis=1, keepdims=True)
    factor = lax.rsqrt(squares / (count * width) + EPS)
    for block in range(count):
        columns = slice(block * width, (block + 1) * width)
        normed[:, columns] = (resid[:, columns] * factor * gain[:, columns]).astype(jnp.bfloat16)
    line.pump(0, 1)
    to_all = exchange(
        "tp", count, lambda _: normed, lambda me: piece.at[me], row_send, row_recv
    )
    for copy in to_all:
        copy.start()
    kept = pltpu.make_async_copy(normed, piece.at[me], local.at[1])
    kept.start()
    for group in range(2):
        for step in range(1, 4):
            if (group, step) != (0, 1):
                line.pump(group, step)
    for copy in to_all:
        copy.wait()
    kept.wait()
    line.finish(0)
    line.finish(1)


ANYWHERE = pl.BlockSpec(memory_space=pl.ANY)
INSIDE = pl.BlockSpec(memory_space=pltpu.VMEM)


def four_of(block):
    return jax.ShapeDtypeStruct((4, *block.shape), block.dtype)


def mix_gather(half, scale):
    line_sems = [pltpu.SemaphoreType.DMA((1, 2, 3, CHUNKS))] * 4
    return pl.pallas_call(
        mix_kernel,
        out_shape=(four_of(half), four_of(half), four_of(scale)),
        in_specs=[ANYWHERE] * 2,
        out_specs=(ANYWHERE,) * 3,
        scratch_shapes=line_sems + [pltpu.SemaphoreType.DMA((3,))] * 2,
        compiler_params=pltpu.CompilerParams(collective_id=0, has_side_effects=True),
    )(half, scale)


def ffn_gather(half_up, half_down, mixed, rows, gain):
    line_sems = [pltpu.SemaphoreType.DMA((2, 2, 3, CHUNKS))] * 4
    few = pltpu.SemaphoreType.DMA((mixed.shape[0] - 1,))
    return pl.pallas_call(
        ffn_kernel,
        out_shape=(
            four_of(half_up),
            four_of(half_up),
            four_of(half_down),
            four_of(half_down),
            jax.ShapeDtypeStruct((mixed.shape[0], *rows.shape), jnp.bfloat16),
            jax.ShapeDtypeStruct(rows.shape, jnp.float32),
        ),
        in_specs=[ANYWHERE, ANYWHERE, INSIDE, INSIDE, INSIDE],
        out_specs=(ANYWHERE,) * 5 + (INSIDE,),
        scratch_shapes=line_sems
        + [
            pltpu.VMEM(mixed.shape, jnp.bfloat16),
            pltpu.VMEM(rows.shape, jnp.bfloat16),
            few,
            few,
            few,
            few,
            pltpu.SemaphoreType.DMA((2,)),
        ],
        compiler_params=pltpu.CompilerParams(collective_id=1, has_side_effects=True),
    )(half_up, half_down, mixed, rows, gain)


def own_half(weight, mine):
    half = weight.shape[0] // 2
    return lax.dynamic_slice_in_dim(weight, mine * half, half, 0)


def arrived_slots(near, far, place):
    pick = lambda blocks, source: lax.dynamic_index_in_dim(blocks, source, 0, keepdims=False)
    return [(pick(near, source), pick(far, source)) for source in line_sources(place)]


def columns_of(rows, start, width):
    return lax.dynamic_slice_in_dim(rows, start, width, 1)


def line_project(rows, own, slots, mine, place):
    width = own.shape[0]
    half = width // 2
    total = dot(columns_of(rows, place * width, width), own)
    for source, (near, far) in zip(line_sources(place), slots):
        total += dot(columns_of(rows, source * width + mine * half, half), near)
        total += dot(columns_of(rows, source * width + (1 - mine) * half, half), far)
    return total


def line_down(hidden, own, slots, scales, mine, place):
    width = own.shape[0]
    half = width // 2
    blocks, starts = [dot_t(hidden, own)], [place * width]
    for source, (near, far) in zip(line_sources(place), slots):
        for block, side in ((near, mine), (far, 1 - mine)):
            blocks.append(dot(hidden, block))
            starts.append(source * width + side * half)
    blocks = [
        (block * lax.dynamic_slice_in_dim(scales, start, block.shape[1], 0)).astype(jnp.bfloat16)
        for block, start in zip(blocks, starts)
    ]
    return blocks, starts


def summed_over_tp(partial_sum, share):
    partial_sum = partial_sum.reshape(-1, share, partial_sum.shape[1])
    pieces = lax.all_to_all(partial_sum, "tp", split_axis=0, concat_axis=0)
    return jnp.sum(pieces.astype(jnp.float32), axis=0)


def shards(
    stream,
    gain_mix,
    w_query,
    scale_query,
    w_key,
    scale_key,
    w_value,
    scale_value,
    gain_ffn,
    w_gate,
    scale_gate,
    w_up,
    scale_up,
    w_down,
    scale_down,
):
    group_rows = stream.shape[0]
    mine = lax.axis_index("rep")
    place = lax.axis_index("fs")
    on_line = (lax.axis_size("rep"), lax.axis_size("fs")) == (2, 4)
    tp_count = lax.axis_size("tp")
    stream_f = stream.astype(jnp.float32)
    normed = (stream_f * rms_scale(stream_f) * gain_mix).astype(jnp.bfloat16)
    mix_w = jnp.concatenate([w.astype(jnp.bfloat16) for w in (w_query, w_key, w_value)], axis=1)
    up_w = jnp.concatenate([w.astype(jnp.bfloat16) for w in (w_gate, w_up)], axis=1)
    down_w = w_down.astype(jnp.bfloat16)
    if on_line:
        near, far, scales = mix_gather(own_half(mix_w, mine), scale_down[None, :])
        scales = lax.dynamic_update_slice(scales, scale_down[None, None, :], (place, 0, 0))
        down_scale = scales.reshape(-1)
        mix_acc = line_project(normed, mix_w, arrived_slots(near, far, place), mine, place)
    else:
        down_scale = lax.all_gather(scale_down, "fs", axis=0, tiled=True)
        mix_acc = dot(normed, lax.all_gather(mix_w, "fs", axis=0, tiled=True))
    mix_scale = jnp.concatenate([scale_query, scale_key, scale_value])
    query, key, value = jnp.split(
        (mix_acc * mix_scale).astype(jnp.bfloat16),
        [w_query.shape[1], w_query.shape[1] + w_key.shape[1]],
        axis=1,
    )
    local_heads = query.shape[1] // DK
    positions = jnp.arange(group_rows, dtype=jnp.int32) % LEN
    mixed = []
    for head in range(local_heads):
        columns = slice(head * DK, (head + 1) * DK)
        queries = rotate(query[:, columns].astype(jnp.float32), positions)
        keys = rotate(key[:, columns].astype(jnp.float32), positions) * DK ** (-0.5)
        values = value[:, head * DV : (head + 1) * DV].astype(jnp.float32)
        head_id = (lax.axis_index("tp") * local_heads + head).astype(jnp.float32)
        log_decay = jnp.log(1.0 - jnp.power(2.0, -5.0 - head_id))
        retained = retention(queries, keys, values, log_decay)
        mixed.append((retained * head_scale(retained)).astype(jnp.bfloat16))
    mixed = jnp.concatenate(mixed, axis=1)
    share = group_rows // tp_count
    own_rows = lax.dynamic_slice_in_dim(stream, lax.axis_index("tp") * share, share, 0)
    if on_line:
        near, far, near_down, far_down, piece, resid = ffn_gather(
            own_half(up_w, mine),
            own_half(down_w, mine).T,
            mixed.reshape(tp_count, share, -1),
            own_rows,
            gain_ffn[None, :],
        )
        piece = piece.reshape(group_rows, -1)
        up_acc = line_project(piece, up_w, arrived_slots(near, far, place), mine, place)
        down_slots = arrived_slots(near_down, far_down, place)
    else:
        arrived = lax.all_to_all(mixed, "tp", split_axis=0, concat_axis=1, tiled=True)
        resid = own_rows.astype(jnp.float32) + arrived.astype(jnp.float32)
        normed_ffn = (resid * rms_scale(resid) * gain_ffn).astype(jnp.bfloat16)
        piece = lax.all_gather(normed_ffn, "tp", axis=0, tiled=True)
        up_acc = dot(piece, lax.all_gather(up_w, "fs", axis=0, tiled=True))
    units = w_gate.shape[1]
    gate = up_acc[:, :units] * scale_gate
    upward = up_acc[:, units:] * scale_up
    hidden = (jax.nn.silu(gate) * upward).astype(jnp.bfloat16)
    if on_line:
        blocks, starts = line_down(hidden, down_w, down_slots, down_scale, mine, place)
        sums = summed_over_tp(jnp.concatenate(blocks, axis=1), share)
        channel_out = jnp.zeros_like(resid)
        offset = 0
        for block, start in zip(blocks, starts):
            width = block.shape[1]
            channel_out = lax.dynamic_update_slice_in_dim(
                channel_out, sums[:, offset : offset + width], start, 1
            )
            offset += width
    else:
        whole = dot_t(hidden, lax.all_gather(down_w, "fs", axis=0, tiled=True))
        channel_out = summed_over_tp((whole * down_scale).astype(jnp.bfloat16), share)
    return (resid + channel_out).astype(jnp.bfloat16)


def solution(mesh):
    placed = (
        P(("rep", "fs"), None),
        P(),
        P("fs", "tp"),
        P("tp"),
        P("fs", "tp"),
        P("tp"),
        P("fs", "tp"),
        P("tp"),
        P(),
        P("fs", "tp"),
        P("tp"),
        P("fs", "tp"),
        P("tp"),
        P("fs", "tp"),
        P("fs"),
    )
    return jax.shard_map(
        shards, mesh=mesh, in_specs=placed, out_specs=P(("rep", "fs", "tp"), None), check_vma=False
    )
```
